128 devices in a mesh: sp: 32 (over z, y, core), tp: 4 (over x).
Axes of the slice: x: 4, y: 4, z: 4, core: 2. Of those that a mesh axis runs over, the one named last changes fastest.
Arguments:
- query_nope: bfloat16 [6144, 4096], P('sp', 'tp'), may hold values from -6 to 6
- query_rope: bfloat16 [6144, 2048], P('sp', 'tp'), may hold values from -24 to 24
- latent: bfloat16 [6144, 512], P('sp'), may hold values from -6 to 6
- key_rope: bfloat16 [6144, 32], P('sp'), may hold values from -24 to 24
- latent_gain: float32 [512], replicated, may hold values from 0.1 to 1.9
- key_up: bfloat16 [512, 4096], P(None, 'tp'), may hold values from -0.25 to 0.25
- value_up: bfloat16 [512, 4096], P(None, 'tp'), may hold values from -0.25 to 0.25
- out_proj: bfloat16 [4096, 4096], P('tp'), may hold values from -0.09375 to 0.09375
- resid: bfloat16 [6144, 4096], P(('sp', 'tp')), may hold values from -6 to 6
- attn_gain: float32 [4096], replicated, may hold values from 0.1 to 1.9
- pre_gain: float32 [4096], replicated, may hold values from 0.1 to 1.9
- routes: int32 [6144, 2], P(('sp', 'tp')), may hold values from 0 to 31, all different within a row; in each aligned block of 48 rows (0 to 47, 48 to 95, ...) at most 6 rows name the same one
- route_weights: float32 [6144, 2], P(('sp', 'tp')), may hold values from 0.2 to 2
- expert_gate: bfloat16 [32, 4096, 1024], P('sp', None, 'tp'), may hold values from -0.09375 to 0.09375
- expert_up: bfloat16 [32, 4096, 1024], P('sp', None, 'tp'), may hold values from -0.09375 to 0.09375
- expert_down: bfloat16 [32, 1024, 4096], P('sp', 'tp'), may hold values from -0.1875 to 0.1875
- shared_gate: bfloat16 [4096, 1024], P(None, 'tp'), may hold values from -0.09375 to 0.09375
- shared_up: bfloat16 [4096, 1024], P(None, 'tp'), may hold values from -0.09375 to 0.09375
- shared_down: bfloat16 [1024, 4096], P('tp'), may hold values from -0.1875 to 0.1875
- moe_gain: float32 [4096], replicated, may hold values from 0.1 to 1.9
Outputs:
- output: bfloat16 [6144, 4096], P(('sp', 'tp'))
The draws below stay inside these ranges and needn't reach their ends.
Inputs may be any that keep to these rules, and one draw needn't show every extreme that they name: `routes`: A row names 2 different experts. In each aligned block of 48 rows no expert is named by more than 6 rows, and in some block an expert is named by exactly 6 rows.
All inputs are finite; a program needn't handle non-finite values.
Results may differ from the reference program's by a relative error of at most 0.018.
Values may be sent and summed in bfloat16 or wider, within the bound.
No kernel may reach another device: no remote copies, remote signals or barrier semaphores. Data moves between devices by JAX's collectives and lax.ppermute only.
A program may use at most 128 MiB of HBM per device.

```python
import math
import jax
import jax.numpy as jnp
import numpy as np
from jax import lax

MODEL_DIM = 4096
HEADS = 64
NOPE_DIM = 64
ROPE_DIM = 32
VALUE_DIM = 64
LATENT = 512
EXPERT_FF = 1024
SHARED_FF = 1024
TOP_K = 2
ROW_DEV = 48
SEQ_LEN = 6144
EXPERTS = 32
CAPACITY = 6
N_TP = 4


def draw_query_rope(key, part):
    drawn_values = jnp.clip(jax.random.normal(jax.random.fold_in(key, 21), (SEQ_LEN, HEADS * ROPE_DIM), jnp.float32), -6.0, 6.0)
    return drawn_values.astype(jnp.bfloat16)


def draw_key_rope(key, part):
    drawn_values = jnp.clip(jax.random.normal(jax.random.fold_in(key, 22), (SEQ_LEN, ROPE_DIM), jnp.float32), -6.0, 6.0)
    return drawn_values.astype(jnp.bfloat16)


def steps_of(rng, extent, pieces, smallest, largest):
    gain = 1.0
    for dim, parts in pieces:
        draws = jax.random.uniform(jax.random.fold_in(jax.random.fold_in(rng, 6), dim), (parts,), jnp.float32, smallest / len(pieces), largest / len(pieces))
        gain = gain * jnp.repeat(jnp.exp(draws), extent[dim] // parts).reshape((-1,) + (1,) * (len(extent) - 1 - dim))
    return gain


def assign_block(stream_key, own, number, rows, amount, top, most, lean):
    ranking = jax.random.permutation(stream_key, amount)
    heavy_load, usual = load_shares(amount, rows * top, most, lean, True), load_shares(amount, rows * top, most, lean, False)
    places = jnp.arange(amount)

    def named(sizes, offset_by):
        used = int((sizes > 0).sum())
        fixed = max(1, used // 4)
        passed = fixed + (places - fixed + offset_by * (used - fixed)) % max(1, amount - fixed)
        return jnp.zeros((amount,), jnp.int32).at[ranking[jnp.where(places < fixed, places, passed)]].set(jnp.asarray(sizes, jnp.int32))

    sizes = jnp.where(number % 4 == 0, named(heavy_load, number // 4), named(usual, number - number // 4 - 1))
    mixed = jax.random.permutation(jax.random.fold_in(own, 3), amount)
    donor, taker = mixed[0:amount // 2 * 2:2], mixed[1:amount // 2 * 2:2]
    room = jnp.minimum(sizes[donor] - 1, most - sizes[taker]) // 2
    room = jnp.where((donor == ranking[0]) | (taker == ranking[0]) | (sizes[taker] == 0), 0, jnp.maximum(room, 0))
    passed = jax.random.randint(jax.random.fold_in(own, 4), (amount // 2,), 0, 1 << 20) % (room + 1)
    sizes = sizes.at[donor].add(-passed).at[taker].add(passed)
    items = jnp.searchsorted(jnp.cumsum(sizes), jnp.arange(rows * top), side="right").astype(jnp.int32)
    table = items.reshape(top, rows).T
    table = table[jax.random.permutation(jax.random.fold_in(own, 1), rows)]
    offset_by = jax.random.randint(jax.random.fold_in(own, 2), (rows, 1), 0, top)
    return jnp.take_along_axis(table, (jnp.arange(top)[None, :] + offset_by) % top, axis=1)


def load_shares(amount, total, reach, slope, full):
    weights = [(1 << 20) // math.isqrt(standing ** slope) + 1 for standing in range(1, amount + 1)]
    largest = reach if full else min(reach, max(-(-total // amount), total * weights[0] // sum(weights)))
    least = 1 if total - largest >= amount - 1 else 0
    counts, spare = [largest] + [least] * (amount - 1), total - largest - least * (amount - 1)
    while spare > 0:
        candidates = [i for i in range(1, amount) if counts[i] < largest] or [i for i in range(1, amount) if counts[i] < reach]
        mass, remaining = sum([weights[i] for i in candidates]), spare
        for i in candidates:
            extra = min(reach - counts[i], max(1, remaining * weights[i] // mass), spare)
            counts[i] = counts[i] + extra
            spare = spare - extra
    return np.array(counts)


def normal_values(own_key, dims, width, reach, pieces=(), kind=jnp.bfloat16):
    array = jax.random.normal(own_key, dims, jnp.float32) * width
    if len(pieces) > 0:
        array = steps_of(own_key, dims, pieces, -0.22, 0.18) * array
    return jnp.clip(array, min=-reach, max=reach).astype(kind)


def setup_inputs(seed: int = 0) -> dict:
    seeds = jax.random.split(jax.random.key(seed), 21)
    query_nope = normal_values(seeds[0], (SEQ_LEN, HEADS * NOPE_DIM), 1.0, 6.0, ((0, 32), (1, 4)))
    query_rope = draw_query_rope(jax.random.fold_in(seeds[20], 71), 0)
    latent = normal_values(seeds[2], (SEQ_LEN, LATENT), 1.0, 6.0, ((0, 32),))
    key_rope = draw_key_rope(jax.random.fold_in(seeds[20], 71), 0)
    latent_gain = jnp.clip(1.0 + 0.18 * jax.random.normal(seeds[4], (LATENT,), jnp.float32), 0.1, 1.9)
    key_up = normal_values(seeds[5], (LATENT, HEADS * NOPE_DIM), LATENT ** -0.5, 0.25, ((1, 4),))
    value_up = normal_values(seeds[6], (LATENT, HEADS * VALUE_DIM), LATENT ** -0.5, 0.25, ((1, 4),))
    out_proj = normal_values(seeds[7], (HEADS * VALUE_DIM, MODEL_DIM), (HEADS * VALUE_DIM) ** -0.5, 0.09375, ((0, 4),))
    resid = normal_values(seeds[8], (SEQ_LEN, MODEL_DIM), 1.0, 6.0, ((0, 128),))
    attn_gain = jnp.clip(1.0 + 0.18 * jax.random.normal(seeds[9], (MODEL_DIM,), jnp.float32), 0.1, 1.9)
    pre_gain = jnp.clip(1.0 + 0.18 * jax.random.normal(seeds[10], (MODEL_DIM,), jnp.float32), 0.1, 1.9)
    routes_keys = jax.random.split(jax.random.fold_in(seeds[11], 1), SEQ_LEN // ROW_DEV)
    routes_turns = jax.random.permutation(jax.random.fold_in(seeds[11], 3), SEQ_LEN // ROW_DEV)
    routes = jax.vmap(lambda own, number: assign_block(jax.random.fold_in(seeds[11], 2), own, number, ROW_DEV, EXPERTS, TOP_K, CAPACITY, 2))(routes_keys, routes_turns).reshape((SEQ_LEN, TOP_K))
    route_weights = jnp.clip(jnp.exp(math.log(2.0) - 2.3025851 * jax.random.uniform(seeds[12], (SEQ_LEN, TOP_K), jnp.float32) ** steps_of(seeds[12], (SEQ_LEN, TOP_K), ((0, 128),), -0.2, 0.2)), 0.2, 2.0)
    expert_gate = normal_values(seeds[13], (EXPERTS, MODEL_DIM, EXPERT_FF), MODEL_DIM ** -0.5, 0.09375, ((0, 32), (2, 4)))
    expert_up = normal_values(seeds[14], (EXPERTS, MODEL_DIM, EXPERT_FF), MODEL_DIM ** -0.5, 0.09375, ((0, 32), (2, 4)))
    expert_down = normal_values(seeds[15], (EXPERTS, EXPERT_FF, MODEL_DIM), EXPERT_FF ** -0.5, 0.1875, ((0, 32), (1, 4)))
    shared_gate = normal_values(seeds[16], (MODEL_DIM, SHARED_FF), MODEL_DIM ** -0.5, 0.09375, ((1, 4),))
    shared_up = normal_values(seeds[17], (MODEL_DIM, SHARED_FF), MODEL_DIM ** -0.5, 0.09375, ((1, 4),))
    shared_down = normal_values(seeds[18], (SHARED_FF, MODEL_DIM), SHARED_FF ** -0.5, 0.1875, ((0, 4),))
    moe_gain = jnp.clip(1.0 + 0.18 * jax.random.normal(seeds[19], (MODEL_DIM,), jnp.float32), 0.1, 1.9)
    return dict(query_nope=query_nope, query_rope=query_rope, latent=latent, key_rope=key_rope, latent_gain=latent_gain, key_up=key_up, value_up=value_up, out_proj=out_proj, resid=resid, attn_gain=attn_gain, pre_gain=pre_gain, routes=routes, route_weights=route_weights, expert_gate=expert_gate, expert_up=expert_up, expert_down=expert_down, shared_gate=shared_gate, shared_up=shared_up, shared_down=shared_down, moe_gain=moe_gain)


epsilon = 1e-06
theta_base = 10000.0

def rms_scale(values, gain_vector):
    return values * lax.rsqrt(lax.optimization_barrier(jnp.mean(values * values, axis=-1, keepdims=True)) + epsilon) * gain_vector

def rotate(values, positions):
    half_dim = values.shape[-1] // 2
    inverse = theta_base ** (-jnp.arange(half_dim, dtype=jnp.float32) / half_dim)
    angles = positions.astype(jnp.float32)[..., None] * inverse
    cosine = jnp.cos(angles)
    sine_part = jnp.sin(angles)
    first_half = values[..., :half_dim]
    second_half = values[..., half_dim:]
    return jnp.concatenate([first_half * cosine - second_half * sine_part, second_half * cosine + first_half * sine_part], axis=-1)

def quarter_product(left_rows, right_cols):
    part_cols = left_rows.shape[1] // N_TP
    result = jnp.zeros((left_rows.shape[0], right_cols.shape[1]), jnp.float32)
    for quarter in range(N_TP):
        partial_value = jnp.dot(left_rows[:, quarter * part_cols:(quarter + 1) * part_cols], right_cols[quarter * part_cols:(quarter + 1) * part_cols], preferred_element_type=jnp.float32)
        rounded = lax.optimization_barrier(partial_value.astype(jnp.bfloat16))
        result = result + rounded.astype(jnp.float32)
    return result

def reference(query_nope, query_rope, latent, key_rope, latent_gain, key_up, value_up, out_proj, resid, attn_gain, pre_gain, routes, route_weights, expert_gate, expert_up, expert_down, shared_gate, shared_up, shared_down, moe_gain):
    positions = jnp.arange(SEQ_LEN, dtype=jnp.int32)
    query_rot = rotate(query_rope.astype(jnp.float32).reshape(SEQ_LEN, HEADS, ROPE_DIM), positions[:, None]).astype(jnp.bfloat16)
    key_rot = rotate(key_rope.astype(jnp.float32), positions).astype(jnp.bfloat16)
    latent_normed = rms_scale(latent.astype(jnp.float32), latent_gain).astype(jnp.bfloat16)
    keys_all = jnp.dot(latent_normed, key_up, preferred_element_type=jnp.float32).astype(jnp.bfloat16)
    keys_all = keys_all.reshape(SEQ_LEN, HEADS, NOPE_DIM).astype(jnp.float32)
    values_all = jnp.dot(latent_normed, value_up, preferred_element_type=jnp.float32).astype(jnp.bfloat16)
    values_all = values_all.reshape(SEQ_LEN, HEADS, VALUE_DIM).astype(jnp.float32)
    query_heads = query_nope.reshape(SEQ_LEN, HEADS, NOPE_DIM).astype(jnp.float32)
    query_rot_f = query_rot.astype(jnp.float32)
    key_rot_f = key_rot.astype(jnp.float32)
    score_scale = (NOPE_DIM + ROPE_DIM) ** (-0.5)
    block_rows = math.gcd(SEQ_LEN, 256)
    outputs = []
    for first_row in range(0, SEQ_LEN, block_rows):
        last_row = first_row + block_rows
        scores = (jnp.einsum('qhd,khd->hqk', query_heads[first_row:last_row], keys_all[:last_row]) + jnp.einsum('qhr,kr->hqk', query_rot_f[first_row:last_row], key_rot_f[:last_row])) * score_scale
        allowed = jnp.arange(last_row)[None, :] <= (first_row + jnp.arange(block_rows))[:, None]
        scores = jnp.where(allowed[None], scores, -jnp.inf)
        row_max = lax.optimization_barrier(jnp.max(scores, axis=-1, keepdims=True))
        exponent = jnp.exp(scores - row_max)
        weights = exponent.astype(jnp.bfloat16).astype(jnp.float32)
        summed = jnp.einsum('hqk,khd->hqd', weights, values_all[:last_row])
        normalized = summed / lax.optimization_barrier(jnp.sum(exponent, axis=-1, keepdims=True))
        outputs.append(normalized.transpose(1, 0, 2).reshape(block_rows, HEADS * VALUE_DIM))
    attention = jnp.concatenate(outputs, axis=0).astype(jnp.bfloat16)
    projected = quarter_product(attention, out_proj)
    mixed = (resid.astype(jnp.float32) + rms_scale(projected, attn_gain)).astype(jnp.bfloat16)
    normed = rms_scale(mixed.astype(jnp.float32), pre_gain).astype(jnp.bfloat16)
    shared_hidden = (jax.nn.silu(jnp.dot(normed, shared_gate, preferred_element_type=jnp.float32)) * jnp.dot(normed, shared_up, preferred_element_type=jnp.float32)).astype(jnp.bfloat16)
    shared_out = quarter_product(shared_hidden, shared_down)
    blocks = SEQ_LEN // ROW_DEV
    flat_routes = routes.reshape(blocks, ROW_DEV * TOP_K)
    onehot = (flat_routes[..., None] == jnp.arange(EXPERTS, dtype=jnp.int32)[None, None, :]).astype(jnp.int32)
    earlier = jnp.cumsum(onehot, axis=1) - onehot
    slot_index = lax.optimization_barrier(jnp.sum(earlier * onehot, axis=-1))
    target = ((jnp.arange(blocks, dtype=jnp.int32)[:, None] * EXPERTS + flat_routes) * CAPACITY + slot_index).reshape(-1)
    source = jnp.arange(SEQ_LEN * TOP_K, dtype=jnp.int32) // TOP_K
    slot_table = jnp.zeros((blocks * EXPERTS * CAPACITY, MODEL_DIM), jnp.bfloat16).at[target].set(normed[source])
    grouped = slot_table.reshape(blocks, EXPERTS, CAPACITY, MODEL_DIM).transpose(1, 0, 2, 3)
    grouped = grouped.reshape(EXPERTS, blocks * CAPACITY, MODEL_DIM)

    def one_expert(operands):
        expert_in, gate_part, up_part, down_part = operands
        hidden = (jax.nn.silu(jnp.dot(expert_in, gate_part, preferred_element_type=jnp.float32)) * jnp.dot(expert_in, up_part, preferred_element_type=jnp.float32)).astype(jnp.bfloat16)
        return quarter_product(hidden, down_part).astype(jnp.bfloat16)
    expert_rows = lax.map(one_expert, (grouped, expert_gate, expert_up, expert_down))
    returned = expert_rows.reshape(EXPERTS, blocks, CAPACITY, MODEL_DIM).transpose(1, 0, 2, 3)
    returned = returned.reshape(blocks * EXPERTS * CAPACITY, MODEL_DIM)
    picked = returned[target].astype(jnp.float32).reshape(SEQ_LEN, TOP_K, MODEL_DIM)
    routed = lax.optimization_barrier(jnp.sum(picked * route_weights[..., None], axis=1))
    moe = shared_out + routed
    return (mixed.astype(jnp.float32) + rms_scale(moe, moe_gain)).astype(jnp.bfloat16)
```

```python
import functools

import jax
import jax.numpy as jnp
from jax import lax
from jax.experimental import pallas as pl
from jax.experimental.pallas import tpu as pltpu
from jax.sharding import PartitionSpec as P


MODEL_DIM = 4096
NOPE_DIM = 64
ROPE_DIM = 32
VALUE_DIM = 64
TOP_K = 2


epsilon = 1e-06
theta_base = 10000.0


def cut_along(array, dim, count):
    before, after = (array.shape[:dim], array.shape[dim + 1 :])
    return jnp.moveaxis(array.reshape(*before, count, -1, *after), dim, 0)


def sum_at_owner(array, axis, dim):
    count = lax.axis_size(axis)
    blocks = lax.all_to_all(cut_along(array, dim, count), axis, 0, 0, tiled=True)
    return jnp.sum(blocks.astype(jnp.float32), axis=0)


def rms_scale(values, gain_vector):
    return (
        values
        * lax.rsqrt(jnp.mean(values * values, axis=-1, keepdims=True) + epsilon)
        * gain_vector
    )


def rotate(values, positions):
    half_dim = values.shape[-1] // 2
    inverse = theta_base ** (-jnp.arange(half_dim, dtype=jnp.float32) / half_dim)
    angles = positions.astype(jnp.float32)[..., None] * inverse
    cosine = jnp.cos(angles)
    sine_part = jnp.sin(angles)
    first_half = values[..., :half_dim]
    second_half = values[..., half_dim:]
    return jnp.concatenate(
        [
            first_half * cosine - second_half * sine_part,
            second_half * cosine + first_half * sine_part,
        ],
        axis=-1,
    )


def gate_kernel(x_ref, w_ref, out_ref):
    out_ref[0] = jnp.dot(x_ref[...], w_ref[0], preferred_element_type=jnp.float32).astype(
        out_ref.dtype
    )


def gate_call(x, weights):
    quarters, _, width = weights.shape
    rows, depth = x.shape
    return pl.pallas_call(
        gate_kernel,
        grid=(quarters,),
        out_shape=jax.ShapeDtypeStruct((quarters, rows, width), jnp.bfloat16),
        in_specs=[
            pl.BlockSpec((rows, depth), lambda q: (0, 0)),
            pl.BlockSpec((1, depth, width), lambda q: (q, 0, 0)),
        ],
        out_specs=pl.BlockSpec((1, rows, width), lambda q: (q, 0, 0)),
        compiler_params=pltpu.CompilerParams(vmem_limit_bytes=40 * 1024 * 1024),
        cost_estimate=pl.CostEstimate(
            flops=2 * rows * depth * width * quarters, bytes_accessed=9_000_000, transcendentals=0
        ),
    )(x, weights)


def down_kernel(hidden_ref, w_ref, routed_ref, shared_ref):
    quarters = hidden_ref.shape[0]
    half = w_ref.shape[1] // 2
    routed_rows = routed_ref.shape[0]
    routed = shared = 0.0
    for q in range(quarters):
        routed += jnp.dot(
            hidden_ref[q, :routed_rows], w_ref[q, :half], preferred_element_type=jnp.float32
        )
        shared += jnp.dot(
            hidden_ref[q, routed_rows:], w_ref[q, half:], preferred_element_type=jnp.float32
        )
    routed_ref[...] = routed.astype(routed_ref.dtype)
    shared_ref[...] = shared


def down_call(hidden, weights, routed_rows, cols):
    quarters, rows, half = hidden.shape
    tile = weights.shape[2]
    first = (weights.shape[1] - 2 * half * cols // tile) // (2 * half)
    return pl.pallas_call(
        down_kernel,
        grid=(cols // tile,),
        out_shape=(
            jax.ShapeDtypeStruct((routed_rows, cols), jnp.bfloat16),
            jax.ShapeDtypeStruct((rows - routed_rows, cols), jnp.float32),
        ),
        in_specs=[
            pl.BlockSpec((quarters, rows, half), lambda n: (0, 0, 0)),
            pl.BlockSpec((quarters, 2 * half, tile), lambda n: (0, first + n, 0)),
        ],
        out_specs=(
            pl.BlockSpec((routed_rows, tile), lambda n: (0, n)),
            pl.BlockSpec((rows - routed_rows, tile), lambda n: (0, n)),
        ),
        compiler_params=pltpu.CompilerParams(vmem_limit_bytes=40 * 1024 * 1024),
        cost_estimate=pl.CostEstimate(
            flops=2 * rows * half * quarters * cols, bytes_accessed=8_000_000, transcendentals=0
        ),
    )(hidden, weights)


def slot_tables(routes, weights, experts, capacity):
    blocks, rows, picks = routes.shape
    flat = routes.reshape(blocks, rows * picks)
    onehot = (flat[..., None] == jnp.arange(experts, dtype=jnp.int32)).astype(jnp.int32)
    earlier = jnp.cumsum(onehot, axis=1) - onehot
    target = flat * (blocks * capacity) + jnp.sum(earlier * onehot, axis=-1)
    target = target + jnp.arange(blocks, dtype=jnp.int32)[:, None] * capacity
    target = target.reshape(blocks * rows, picks)
    slots = jnp.arange(experts * blocks * capacity, dtype=jnp.int32)
    spread = jnp.any(target.T[:, None, :] == slots[None, :, None], axis=0).astype(jnp.bfloat16)
    shares = jnp.sum(
        jnp.where(
            target[:, :, None] == slots[None, None, :],
            weights.reshape(blocks * rows, picks)[..., None],
            0.0,
        ),
        axis=1,
    )
    high = lax.reduce_precision(shares, 8, 7)
    return spread, high.astype(jnp.bfloat16), (shares - high).astype(jnp.bfloat16)


def far_pairs(groups, pairs):
    counts = []
    for low in range(groups // 2):
        mine, theirs = low // 2 + 2.1, (groups - 1 - low) // 2 + 2.1
        best = min(
            range(pairs // 2 + 1),
            key=lambda n: max(pairs * mine + n * theirs, (pairs - n) * theirs),
        )
        counts.append(best)
    return counts


LOG2E = 1.4426950408889634
PACK_ROWS = 16


def attention_kernel(
    desc_ref, gath_ref, qt_ref, ku_ref, vu_ref, out_ref, rot_ref, w_ref, *, block, score_scale
):
    devices, grows, lat_dim = gath_ref.shape
    rows = grows - PACK_ROWS
    per = block // rows
    width = qt_ref.shape[2]
    half = width // 2
    factor = score_scale * LOG2E
    rot_ref[...] = jnp.zeros_like(rot_ref)

    def unpack(d, _):
        packed = gath_ref[d, rows:grows, :]
        for g in range(rows // PACK_ROWS):
            rot_ref[d, g * PACK_ROWS : (g + 1) * PACK_ROWS, 0:ROPE_DIM] = packed[
                :, g * ROPE_DIM : (g + 1) * ROPE_DIM
            ]
        return 0

    lax.fori_loop(0, devices, unpack, 0)
    n_own, i_own, n_far, i_far = desc_ref[0], desc_ref[1], desc_ref[2], desc_ref[3]
    pairs = ku_ref.shape[1] // 128
    extra = qt_ref.shape[0] - pairs

    def one_pair(u, _):
        far = u >= n_own
        pair = jnp.where(far, pairs - n_far + (u - n_own), u)
        slot = jnp.where(far, pair + extra, pair)
        index = jnp.where(far, i_far, i_own)
        col = pl.multiple_of(pair * 128, 128)
        w_ref[:, 0:128] = ku_ref[:, pl.ds(col, 128)]
        w_ref[:, 128:256] = vu_ref[:, pl.ds(col, 128)]

        def scores(b):
            lat = gath_ref[pl.ds(b * per, per), 0:rows, :].reshape(block, lat_dim)
            kv = jnp.dot(lat, w_ref[...], preferred_element_type=jnp.float32).astype(jnp.bfloat16)
            rot = rot_ref[pl.ds(b * per, per)].reshape(block, 128)
            keys = jnp.concatenate([kv[:, :128], rot], axis=1)
            s = jnp.dot(keys, qt_ref[slot], preferred_element_type=jnp.float32)
            return s, kv[:, 128:]

        def weigh(v, p):
            return lax.dot_general(
                v,
                p.astype(jnp.bfloat16),
                (((0,), (0,)), ((), ())),
                preferred_element_type=jnp.float32,
            )

        full = (index * rows) // block
        s, v = scores(full)
        key = lax.broadcasted_iota(jnp.int32, (block, width), 0) + full * block
        lane = lax.broadcasted_iota(jnp.int32, (block, width), 1)
        query = index * rows + jnp.where(lane >= half, lane - half, lane)
        s = jnp.where(key <= query, s, -1e30)
        top = jnp.max(s, axis=0, keepdims=True)
        p = jnp.exp2(s * factor - top * factor)
        state = (top, jnp.sum(p, axis=0, keepdims=True), weigh(v, p))

        def update(state, s, v):
            top, total, acc = state
            newest = jnp.maximum(top, jnp.max(s, axis=0, keepdims=True))
            alpha = jnp.exp2((top - newest) * factor)
            p = jnp.exp2(s * factor - newest * factor)
            total = total * alpha + jnp.sum(p, axis=0, keepdims=True)
            return newest, total, acc * alpha + weigh(v, p)

        def two(b, state):
            first, second = scores(b * 2), scores(b * 2 + 1)
            return update(update(state, *first), *second)

        state = lax.fori_loop(0, full // 2, two, state)
        state = lax.fori_loop(
            (full // 2) * 2, full, lambda b, state: update(state, *scores(b)), state
        )
        top, total, acc = state
        res = acc / total
        out_ref[slot, 0:64, :] = res[0:64, 0:half].astype(jnp.bfloat16)
        out_ref[slot, 64:128, :] = res[64:128, half:].astype(jnp.bfloat16)
        return 0

    lax.fori_loop(0, n_own + n_far, one_pair, 0)


def attention_call(desc, gathered, qt, key_up, value_up, score_scale):
    devices, grows, lat_dim = gathered.shape
    rows = grows - PACK_ROWS
    slots, _, width = qt.shape
    return pl.pallas_call(
        functools.partial(attention_kernel, block=rows * 2, score_scale=score_scale),
        out_shape=jax.ShapeDtypeStruct((slots, 128, width // 2), jnp.bfloat16),
        in_specs=[pl.BlockSpec(memory_space=pltpu.SMEM)]
        + [pl.BlockSpec(memory_space=pltpu.VMEM)] * 4,
        out_specs=pl.BlockSpec(memory_space=pltpu.VMEM),
        scratch_shapes=[
            pltpu.VMEM((devices, rows, 128), jnp.bfloat16),
            pltpu.VMEM((lat_dim, 256), jnp.bfloat16),
        ],
        compiler_params=pltpu.CompilerParams(vmem_limit_bytes=50 * 1024 * 1024),
        cost_estimate=pl.CostEstimate(
            flops=50_000_000_000, bytes_accessed=12_000_000, transcendentals=20_000_000
        ),
    )(desc, gathered, qt, key_up, value_up)


def query_tiles(query_nope, query_rot):
    rows = query_nope.shape[0]
    pairs = query_nope.shape[1] // (2 * NOPE_DIM)
    nope = query_nope.reshape(rows, pairs, 2, NOPE_DIM).transpose(1, 2, 3, 0)
    rot = query_rot.reshape(rows, pairs, 2, ROPE_DIM).transpose(1, 2, 3, 0)
    none = jnp.zeros_like(nope[:, 0])
    return jnp.concatenate(
        [
            jnp.concatenate([nope[:, 0], none], axis=2),
            jnp.concatenate([none, nope[:, 1]], axis=2),
            jnp.concatenate([rot[:, 0], rot[:, 1]], axis=2),
            jnp.zeros((pairs, 128 - ROPE_DIM, 2 * rows), query_nope.dtype),
        ],
        axis=1,
    )


def layer(
    query_nope,
    query_rope,
    latent,
    key_rope,
    latent_gain,
    key_up,
    value_up,
    out_proj,
    resid,
    attn_gain,
    pre_gain,
    routes,
    route_weights,
    expert_gate,
    expert_up,
    expert_down,
    shared_gate,
    shared_up,
    shared_down,
    moe_gain,
):
    local_rows = query_nope.shape[0]
    heads_here = query_nope.shape[1] // NOPE_DIM
    query_pos = lax.axis_index("sp") * local_rows + jnp.arange(local_rows, dtype=jnp.int32)
    query_rot = rotate(
        query_rope.astype(jnp.float32).reshape(local_rows, heads_here, ROPE_DIM), query_pos[:, None]
    ).astype(jnp.bfloat16)
    key_rot = rotate(key_rope.astype(jnp.float32), query_pos).astype(jnp.bfloat16)
    latent_normed = rms_scale(latent.astype(jnp.float32), latent_gain).astype(jnp.bfloat16)
    score_scale = (NOPE_DIM + ROPE_DIM) ** (-0.5)

    groups = lax.axis_size("sp")
    place = lax.axis_index("sp").astype(jnp.int32)
    tp_count = lax.axis_size("tp")
    pairs = heads_here // 2
    far = pairs // 2
    cols = MODEL_DIM // tp_count
    rows_here = resid.shape[0]
    capacity = max(2, 2 * rows_here * TOP_K // groups)
    group_rows = tp_count * rows_here

    sent_queries = jnp.concatenate(
        [
            query_nope[:, far * 2 * NOPE_DIM :],
            query_rot.reshape(local_rows, -1)[:, far * 2 * ROPE_DIM :],
        ],
        axis=1,
    )
    down_pairs = [(groups - 1 - low, low) for low in range(groups // 2)]
    far_queries = lax.ppermute(sent_queries, "sp", down_pairs)

    packed_rot = key_rot.reshape(local_rows // PACK_ROWS, PACK_ROWS, ROPE_DIM).transpose(1, 0, 2)
    packed_rot = packed_rot.reshape(PACK_ROWS, -1)
    packed_rot = jnp.pad(packed_rot, ((0, 0), (0, latent.shape[1] - packed_rot.shape[1])))
    gathered = lax.all_gather(
        jnp.concatenate([latent_normed, packed_rot], axis=0), "sp", axis=0, tiled=False
    )

    route_data = lax.all_gather(
        jnp.concatenate([routes.astype(jnp.float32), route_weights], axis=1), "tp", axis=0
    )
    gate_up = jnp.concatenate([expert_gate[0], expert_up[0]], axis=1)
    gate_width = gate_up.shape[1]
    gate_up = gate_up.reshape(tp_count, cols, gate_width)
    downs = jnp.concatenate([expert_down[0], shared_down], axis=0)
    downs = downs.reshape(downs.shape[0], tp_count, cols // gate_width, gate_width)
    downs = downs.transpose(1, 2, 0, 3).reshape(tp_count, -1, gate_width)
    gate_up, downs, route_data = lax.optimization_barrier((gate_up, downs, route_data))
    weights = lax.all_to_all(
        jnp.concatenate([gate_up, downs], axis=1), "tp", split_axis=0, concat_axis=0, tiled=True
    )
    spread, share_high, share_low = slot_tables(
        route_data[..., :TOP_K].astype(jnp.int32), route_data[..., TOP_K:], groups, capacity
    )

    is_low = place < groups // 2
    low_place = jnp.minimum(place, groups - 1 - place)
    moved = jnp.asarray(far_pairs(groups, pairs), jnp.int32)[low_place]
    n_own = jnp.where(is_low, pairs, pairs - moved)
    desc = jnp.stack([n_own, place, jnp.where(is_low, moved, 0), groups - 1 - place])
    tiles = jnp.concatenate(
        [
            query_tiles(query_nope, query_rot),
            query_tiles(
                far_queries[:, : far * 2 * NOPE_DIM], far_queries[:, far * 2 * NOPE_DIM :]
            ),
        ],
        axis=0,
    )
    desc, spread, share_high, share_low = lax.optimization_barrier(
        (desc, spread, share_high, share_low)
    )
    attended = attention_call(desc, gathered, tiles, key_up, value_up, score_scale)
    returned = lax.ppermute(attended[pairs:], "sp", [(low, high) for high, low in down_pairs])
    pair_ids = jnp.arange(pairs - far, pairs, dtype=jnp.int32)[:, None, None]
    attended = jnp.concatenate(
        [
            attended[: pairs - far],
            jnp.where(pair_ids < n_own, attended[pairs - far : pairs], returned),
        ],
        axis=0,
    ).reshape(heads_here * VALUE_DIM, local_rows)
    partial = lax.dot_general(
        attended, out_proj, (((0,), (0,)), ((), ())), preferred_element_type=jnp.float32
    ).astype(jnp.bfloat16)
    projected = sum_at_owner(partial, "tp", 0)
    mixed = (resid.astype(jnp.float32) + rms_scale(projected, attn_gain)).astype(jnp.bfloat16)
    normed = rms_scale(mixed.astype(jnp.float32), pre_gain).astype(jnp.bfloat16)

    columns = lax.all_to_all(
        normed.reshape(rows_here, tp_count, cols).transpose(1, 0, 2),
        "tp",
        split_axis=0,
        concat_axis=0,
        tiled=True,
    ).reshape(group_rows, cols)
    group_normed = lax.all_gather(normed, "tp", axis=0, tiled=True)
    table = jnp.dot(spread, columns, preferred_element_type=jnp.float32).astype(jnp.bfloat16)
    slots = table.shape[0]
    arrived = lax.all_to_all(
        table.reshape(groups, -1, cols), "sp", split_axis=0, concat_axis=0, tiled=True
    ).reshape(slots, cols)
    partial = gate_call(arrived, weights)
    gated = lax.psum_scatter(partial, "tp", scatter_dimension=0, tiled=False).astype(jnp.float32)
    width = gated.shape[1] // 2
    routed_hidden = (jax.nn.silu(gated[:, :width]) * gated[:, width:]).astype(jnp.bfloat16)
    shared_hidden = (
        jax.nn.silu(jnp.dot(group_normed, shared_gate, preferred_element_type=jnp.float32))
        * jnp.dot(group_normed, shared_up, preferred_element_type=jnp.float32)
    ).astype(jnp.bfloat16)
    hidden = lax.all_gather(
        jnp.concatenate([routed_hidden, shared_hidden], axis=0), "tp", axis=0, tiled=False
    )
    routed_out, shared_out = down_call(hidden, weights, slots, cols)
    expert_rows = lax.all_to_all(
        routed_out.reshape(groups, -1, cols), "sp", split_axis=0, concat_axis=0, tiled=True
    ).reshape(slots, cols)
    moe = (
        shared_out
        + jnp.dot(share_high, expert_rows, preferred_element_type=jnp.float32)
        + jnp.dot(share_low, expert_rows, preferred_element_type=jnp.float32)
    )
    moe = lax.all_to_all(
        moe.astype(jnp.bfloat16).reshape(tp_count, rows_here, cols),
        "tp",
        split_axis=0,
        concat_axis=0,
        tiled=True,
    )
    moe = moe.transpose(1, 0, 2).reshape(rows_here, MODEL_DIM).astype(jnp.float32)
    return (mixed.astype(jnp.float32) + rms_scale(moe, moe_gain)).astype(jnp.bfloat16)


def solution(mesh):
    in_specs = (
        P("sp", "tp"),
        P("sp", "tp"),
        P("sp", None),
        P("sp", None),
        P(),
        P(None, "tp"),
        P(None, "tp"),
        P("tp", None),
        P(("sp", "tp"), None),
        P(),
        P(),
        P(("sp", "tp"), None),
        P(("sp", "tp"), None),
        P("sp", None, "tp"),
        P("sp", None, "tp"),
        P("sp", "tp", None),
        P(None, "tp"),
        P(None, "tp"),
        P("tp", None),
        P(),
    )
    out_specs = P(("sp", "tp"), None)
    return jax.shard_map(layer, mesh=mesh, in_specs=in_specs, out_specs=out_specs, check_vma=False)
```

```python
import functools

import jax
import jax.numpy as jnp
from jax import lax
from jax.experimental import pallas as pl
from jax.experimental.pallas import tpu as pltpu
from jax.sharding import PartitionSpec as P


MODEL_DIM = 4096
NOPE_DIM = 64
ROPE_DIM = 32
TOP_K = 2


epsilon = 1e-06
theta_base = 10000.0


def cut_along(array, dim, count):
    before, after = (array.shape[:dim], array.shape[dim + 1 :])
    return jnp.moveaxis(array.reshape(*before, count, -1, *after), dim, 0)


def sum_at_owner(array, axis, dim):
    count = lax.axis_size(axis)
    blocks = lax.all_to_all(cut_along(array, dim, count), axis, 0, 0, tiled=True)
    return jnp.sum(blocks.astype(jnp.float32), axis=0)


def rms_scale(values, gain_vector):
    return (
        values
        * lax.rsqrt(jnp.mean(values * values, axis=-1, keepdims=True) + epsilon)
        * gain_vector
    )


def rotate(values, positions):
    half_dim = values.shape[-1] // 2
    inverse = theta_base ** (-jnp.arange(half_dim, dtype=jnp.float32) / half_dim)
    angles = positions.astype(jnp.float32)[..., None] * inverse
    cosine = jnp.cos(angles)
    sine_part = jnp.sin(angles)
    first_half = values[..., :half_dim]
    second_half = values[..., half_dim:]
    return jnp.concatenate(
        [
            first_half * cosine - second_half * sine_part,
            second_half * cosine + first_half * sine_part,
        ],
        axis=-1,
    )


def project_kernel(own_ref, attended_ref, returned_ref, w_ref, out_ref, x_ref):
    pairs = x_ref.shape[1] // 128
    kept = pairs - returned_ref.shape[0]

    @pl.when(pl.program_id(0) == 0)
    def _():
        for pair in range(pairs):
            x = attended_ref[pair]
            if pair >= kept:
                x = jnp.where(pair < own_ref[0], x, returned_ref[pair - kept])
            x_ref[:, pair * 128 : (pair + 1) * 128] = x.astype(jnp.float32).T.astype(jnp.bfloat16)

    out_ref[...] = jnp.dot(x_ref[...], w_ref[...], preferred_element_type=jnp.float32).astype(
        out_ref.dtype
    )


def project_call(own, attended, returned, weights):
    depth, cols = weights.shape
    rows = attended.shape[2]
    tile = cols // 8
    return pl.pallas_call(
        project_kernel,
        grid=(cols // tile,),
        out_shape=jax.ShapeDtypeStruct((rows, cols), jnp.bfloat16),
        in_specs=[
            pl.BlockSpec(memory_space=pltpu.SMEM),
            pl.BlockSpec(attended.shape, lambda n: (0, 0, 0)),
            pl.BlockSpec(returned.shape, lambda n: (0, 0, 0)),
            pl.BlockSpec((depth, tile), lambda n: (0, n)),
        ],
        out_specs=pl.BlockSpec((rows, tile), lambda n: (0, n)),
        scratch_shapes=[pltpu.VMEM((rows, depth), jnp.bfloat16)],
        compiler_params=pltpu.CompilerParams(vmem_limit_bytes=20 * 1024 * 1024),
        cost_estimate=pl.CostEstimate(
            flops=2 * rows * depth * cols, bytes_accessed=11_000_000, transcendentals=0
        ),
    )(own, attended, returned, weights)


def pack_kernel(gate_ref, up_ref, down_ref, out_ref):
    cols, width = gate_ref.shape[1], gate_ref.shape[2]
    depth, tile = down_ref.shape[1], out_ref.shape[2]
    out_ref[0, 0:cols, 0:width] = gate_ref[0]
    out_ref[0, 0:cols, width : 2 * width] = up_ref[0]
    for half in range(cols // tile):
        row = cols + half * depth
        out_ref[0, row : row + depth] = down_ref[0, :, half * tile : (half + 1) * tile]


def pack_call(gate, up, down, quarters):
    cols = gate.shape[1] // quarters
    width, depth = gate.shape[2], down.shape[1]
    rows = cols + depth * cols // (2 * width)
    return pl.pallas_call(
        pack_kernel,
        grid=(quarters,),
        out_shape=jax.ShapeDtypeStruct((quarters, rows, 2 * width), gate.dtype),
        in_specs=[
            pl.BlockSpec((1, cols, width), lambda q: (0, q, 0)),
            pl.BlockSpec((1, cols, width), lambda q: (0, q, 0)),
            pl.BlockSpec((1, depth, cols), lambda q: (0, 0, q)),
        ],
        out_specs=pl.BlockSpec((1, rows, 2 * width), lambda q: (q, 0, 0)),
        compiler_params=pltpu.CompilerParams(vmem_limit_bytes=56 * 1024 * 1024),
        cost_estimate=pl.CostEstimate(flops=0, bytes_accessed=13_000_000, transcendentals=0),
    )(gate, up, down)


def gate_kernel(x_ref, w_ref, out_ref):
    out_ref[0] = jnp.dot(x_ref[...], w_ref[0], preferred_element_type=jnp.float32).astype(
        out_ref.dtype
    )


def gate_call(x, weights):
    quarters, _, width = weights.shape
    rows, depth = x.shape
    return pl.pallas_call(
        gate_kernel,
        grid=(quarters,),
        out_shape=jax.ShapeDtypeStruct((quarters, rows, width), jnp.bfloat16),
        in_specs=[
            pl.BlockSpec((rows, depth), lambda q: (0, 0)),
            pl.BlockSpec((1, depth, width), lambda q: (q, 0, 0)),
        ],
        out_specs=pl.BlockSpec((1, rows, width), lambda q: (q, 0, 0)),
        compiler_params=pltpu.CompilerParams(vmem_limit_bytes=56 * 1024 * 1024),
        cost_estimate=pl.CostEstimate(
            flops=2 * rows * depth * width * quarters, bytes_accessed=9_000_000, transcendentals=0
        ),
    )(x, weights)


def down_kernel(first_ref, second_ref, w_ref, routed_ref):
    quarters, middle, _ = first_ref.shape

    def total(ref):
        return sum(
            jnp.dot(ref[q], w_ref[q], preferred_element_type=jnp.float32) for q in range(quarters)
        )

    routed_ref[:middle] = total(first_ref).astype(routed_ref.dtype)
    routed_ref[middle:] = total(second_ref).astype(routed_ref.dtype)


def down_call(first_half, second_half, weights, cols):
    quarters, middle, half = first_half.shape
    tile = weights.shape[2]
    first = weights.shape[1] // half - cols // tile
    return pl.pallas_call(
        down_kernel,
        grid=(cols // tile,),
        out_shape=jax.ShapeDtypeStruct((2 * middle, cols), jnp.bfloat16),
        in_specs=[
            pl.BlockSpec((quarters, middle, half), lambda n: (0, 0, 0)),
            pl.BlockSpec((quarters, middle, half), lambda n: (0, 0, 0)),
            pl.BlockSpec((quarters, half, tile), lambda n: (0, first + n, 0)),
        ],
        out_specs=pl.BlockSpec((2 * middle, tile), lambda n: (0, n)),
        compiler_params=pltpu.CompilerParams(vmem_limit_bytes=24 * 1024 * 1024),
        cost_estimate=pl.CostEstimate(
            flops=4 * middle * half * quarters * cols, bytes_accessed=8_000_000, transcendentals=0
        ),
    )(first_half, second_half, weights)


def slot_tables(routes, weights, experts, capacity):
    blocks, rows, picks = routes.shape
    flat = routes.reshape(blocks, rows * picks)
    onehot = (flat[..., None] == jnp.arange(experts, dtype=jnp.int32)).astype(jnp.int32)
    earlier = jnp.cumsum(onehot, axis=1) - onehot
    target = flat * (blocks * capacity) + jnp.sum(earlier * onehot, axis=-1)
    target = target + jnp.arange(blocks, dtype=jnp.int32)[:, None] * capacity
    target = target.reshape(blocks * rows, picks)
    slots = jnp.arange(experts * blocks * capacity, dtype=jnp.int32)
    spread = jnp.any(target.T[:, None, :] == slots[None, :, None], axis=0).astype(jnp.bfloat16)
    shares = jnp.sum(
        jnp.where(
            target[:, :, None] == slots[None, None, :],
            weights.reshape(blocks * rows, picks)[..., None],
            0.0,
        ),
        axis=1,
    )
    high = lax.reduce_precision(shares, 8, 7)
    return spread, high.astype(jnp.bfloat16), (shares - high).astype(jnp.bfloat16)


def far_pairs(groups, pairs):
    counts = []
    for low in range(groups // 2):
        mine, theirs = low + 5.6, groups + 4.6 - low
        best = min(
            range(pairs // 2 + 1),
            key=lambda n: max(pairs * mine + n * theirs, (pairs - n) * theirs),
        )
        counts.append(best)
    return counts


LOG2E = 1.4426950408889634
PACK_ROWS = 16
CHAINS = (10, 5, 2, 1)
ATTEND_VMEM = 44


def attention_kernel(
    desc_ref, gath_ref, qt_ref, ku_ref, vu_ref, out_ref, rot_ref, w_ref, *, block, score_scale
):
    devices, grows, lat_dim = gath_ref.shape
    rows = grows - PACK_ROWS
    per = block // rows
    width = qt_ref.shape[2]
    half = width // 2
    factor = score_scale * LOG2E
    rot_ref[...] = jnp.zeros_like(rot_ref)

    def unpack(d, _):
        packed = gath_ref[d, rows:grows, :]
        for g in range(rows // PACK_ROWS):
            rot_ref[d, g * PACK_ROWS : (g + 1) * PACK_ROWS, 0:ROPE_DIM] = packed[
                :, g * ROPE_DIM : (g + 1) * ROPE_DIM
            ]
        return 0

    lax.fori_loop(0, devices, unpack, 0)
    n_own, i_own, n_far, i_far = desc_ref[0], desc_ref[1], desc_ref[2], desc_ref[3]
    pairs = ku_ref.shape[1] // 128
    extra = qt_ref.shape[0] - pairs

    def one_pair(u, _):
        far = u >= n_own
        pair = jnp.where(far, pairs - n_far + (u - n_own), u)
        slot = jnp.where(far, pair + extra, pair)
        index = jnp.where(far, i_far, i_own)
        col = pl.multiple_of(pair * 128, 128)
        w_ref[:, 0:128] = ku_ref[:, pl.ds(col, 128)]
        w_ref[:, 128:256] = vu_ref[:, pl.ds(col, 128)]

        count_all = index + 1
        row = lax.broadcasted_iota(jnp.int32, (block, width), 0)
        lane = lax.broadcasted_iota(jnp.int32, (block, width), 1)
        ahead = row - jnp.where(lane >= half, lane - half, lane) - index * rows
        state = (
            jnp.full((1, width), -1e30, jnp.float32),
            jnp.zeros((1, width), jnp.float32),
            jnp.zeros((128, width), jnp.float32),
        )

        def scores(b):
            lat = gath_ref[pl.ds(b * per, per), 0:rows, :].reshape(block, lat_dim)
            kv = jnp.dot(lat, w_ref[...], preferred_element_type=jnp.float32).astype(jnp.bfloat16)
            rot = rot_ref[pl.ds(b * per, per)].reshape(block, 128)
            keys = jnp.concatenate([kv[:, :128], rot], axis=1)
            s = jnp.dot(keys, qt_ref[slot], preferred_element_type=jnp.float32)
            return jnp.where(ahead <= -b * block, s, -1e30), kv[:, 128:]

        def weigh(v, p):
            return lax.dot_general(
                v,
                p.astype(jnp.bfloat16),
                (((0,), (0,)), ((), ())),
                preferred_element_type=jnp.float32,
            )

        def update(state, s, v):
            top, total, acc = state
            newest = jnp.maximum(top, jnp.max(s, axis=0, keepdims=True))
            alpha = jnp.exp2((top - newest) * factor)
            p = jnp.exp2(s * factor - newest * factor)
            total = total * alpha + jnp.sum(p, axis=0, keepdims=True)
            return newest, total, acc * alpha + weigh(v, p)

        def several(count):
            def body(_, carry):
                start, state = carry
                found = [scores(start + k) for k in range(count)]
                for pair_scores in found:
                    state = update(state, *pair_scores)
                return start + count, state

            return body

        carry, left = (jnp.int32(0), state), count_all
        for count in CHAINS:
            carry = lax.fori_loop(0, left // count, several(count), carry)
            left = left % count
        _, total, acc = carry[1]
        res = acc / total
        out_ref[slot, 0:64, :] = res[0:64, 0:half].astype(jnp.bfloat16)
        out_ref[slot, 64:128, :] = res[64:128, half:].astype(jnp.bfloat16)
        return 0

    lax.fori_loop(0, n_own + n_far, one_pair, 0)


def attention_call(desc, gathered, qt, key_up, value_up, score_scale):
    devices, grows, lat_dim = gathered.shape
    rows = grows - PACK_ROWS
    slots, _, width = qt.shape
    return pl.pallas_call(
        functools.partial(attention_kernel, block=rows, score_scale=score_scale),
        out_shape=jax.ShapeDtypeStruct((slots, 128, width // 2), jnp.bfloat16),
        in_specs=[pl.BlockSpec(memory_space=pltpu.SMEM)]
        + [pl.BlockSpec(memory_space=pltpu.VMEM)] * 4,
        out_specs=pl.BlockSpec(memory_space=pltpu.VMEM),
        scratch_shapes=[
            pltpu.VMEM((devices, rows, 128), jnp.bfloat16),
            pltpu.VMEM((lat_dim, 256), jnp.bfloat16),
        ],
        compiler_params=pltpu.CompilerParams(vmem_limit_bytes=ATTEND_VMEM * 1024 * 1024),
        cost_estimate=pl.CostEstimate(
            flops=50_000_000_000, bytes_accessed=12_000_000, transcendentals=20_000_000
        ),
    )(desc, gathered, qt, key_up, value_up)


def query_tiles(query_nope, query_rot):
    rows = query_nope.shape[0]
    pairs = query_nope.shape[1] // (2 * NOPE_DIM)
    nope = query_nope.reshape(rows, pairs, 2, NOPE_DIM).transpose(1, 2, 3, 0)
    rot = query_rot.reshape(rows, pairs, 2, ROPE_DIM).transpose(1, 2, 3, 0)
    none = jnp.zeros_like(nope[:, 0])
    return jnp.concatenate(
        [
            jnp.concatenate([nope[:, 0], none], axis=2),
            jnp.concatenate([none, nope[:, 1]], axis=2),
            jnp.concatenate([rot[:, 0], rot[:, 1]], axis=2),
            jnp.zeros((pairs, 128 - ROPE_DIM, 2 * rows), query_nope.dtype),
        ],
        axis=1,
    )


def layer(
    query_nope,
    query_rope,
    latent,
    key_rope,
    latent_gain,
    key_up,
    value_up,
    out_proj,
    resid,
    attn_gain,
    pre_gain,
    routes,
    route_weights,
    expert_gate,
    expert_up,
    expert_down,
    shared_gate,
    shared_up,
    shared_down,
    moe_gain,
):
    local_rows = query_nope.shape[0]
    heads_here = query_nope.shape[1] // NOPE_DIM
    query_pos = lax.axis_index("sp") * local_rows + jnp.arange(local_rows, dtype=jnp.int32)
    query_rot = rotate(
        query_rope.astype(jnp.float32).reshape(local_rows, heads_here, ROPE_DIM), query_pos[:, None]
    ).astype(jnp.bfloat16)
    key_rot = rotate(key_rope.astype(jnp.float32), query_pos).astype(jnp.bfloat16)
    latent_normed = rms_scale(latent.astype(jnp.float32), latent_gain).astype(jnp.bfloat16)
    score_scale = (NOPE_DIM + ROPE_DIM) ** (-0.5)

    groups = lax.axis_size("sp")
    place = lax.axis_index("sp").astype(jnp.int32)
    tp_count = lax.axis_size("tp")
    pairs = heads_here // 2
    counts = far_pairs(groups, pairs)
    far = max(1, max(counts))
    cols = MODEL_DIM // tp_count
    rows_here = resid.shape[0]
    capacity = max(2, 2 * rows_here * TOP_K // groups)
    group_rows = tp_count * rows_here

    sent_queries = jnp.concatenate(
        [
            query_nope[:, (pairs - far) * 2 * NOPE_DIM :],
            query_rot.reshape(local_rows, -1)[:, (pairs - far) * 2 * ROPE_DIM :],
        ],
        axis=1,
    )
    down_pairs = [(groups - 1 - low, low) for low in range(groups // 2)]
    far_queries = lax.ppermute(sent_queries, "sp", down_pairs)

    packed_rot = key_rot.reshape(local_rows // PACK_ROWS, PACK_ROWS, ROPE_DIM).transpose(1, 0, 2)
    packed_rot = packed_rot.reshape(PACK_ROWS, -1)
    packed_rot = jnp.pad(packed_rot, ((0, 0), (0, latent.shape[1] - packed_rot.shape[1])))
    gathered = lax.all_gather(
        jnp.concatenate([latent_normed, packed_rot], axis=0), "sp", axis=0, tiled=False
    )

    own_routes = jnp.concatenate([routes.astype(jnp.float32), route_weights], axis=1)
    turn = lax.axis_index("tp")
    parts = [own_routes] + [
        lax.ppermute(own_routes, "tp", [(d, (d + k) % tp_count) for d in range(tp_count)])
        for k in range(1, tp_count)
    ]
    owner = jnp.arange(tp_count, dtype=jnp.int32)[:, None, None]
    route_data = sum(
        jnp.where(owner == (turn - k) % tp_count, part[None], 0.0) for k, part in enumerate(parts)
    )
    packed = pack_call(expert_gate, expert_up, expert_down, tp_count)
    weights = lax.all_to_all(packed, "tp", split_axis=0, concat_axis=0, tiled=True)
    spread, share_high, share_low = slot_tables(
        route_data[..., :TOP_K].astype(jnp.int32), route_data[..., TOP_K:], groups, capacity
    )

    is_low = place < groups // 2
    low_place = jnp.minimum(place, groups - 1 - place)
    moved = jnp.asarray(counts, jnp.int32)[low_place]
    n_own = jnp.where(is_low, pairs, pairs - moved)
    desc = jnp.stack([n_own, place, jnp.where(is_low, moved, 0), groups - 1 - place])
    tiles = jnp.concatenate(
        [
            query_tiles(query_nope, query_rot),
            query_tiles(
                far_queries[:, : far * 2 * NOPE_DIM], far_queries[:, far * 2 * NOPE_DIM :]
            ),
        ],
        axis=0,
    )
    desc, spread, share_high, share_low = lax.optimization_barrier(
        (desc, spread, share_high, share_low)
    )
    attended = attention_call(desc, gathered, tiles, key_up, value_up, score_scale)
    returned = lax.ppermute(attended[pairs:], "sp", [(low, high) for high, low in down_pairs])
    partial = project_call(n_own.reshape(1), attended, returned, out_proj)
    projected = sum_at_owner(partial, "tp", 0)
    mixed = (resid.astype(jnp.float32) + rms_scale(projected, attn_gain)).astype(jnp.bfloat16)
    normed = rms_scale(mixed.astype(jnp.float32), pre_gain).astype(jnp.bfloat16)

    columns = lax.all_to_all(
        jnp.stack([normed[:, q * cols : (q + 1) * cols] for q in range(tp_count)]),
        "tp",
        split_axis=0,
        concat_axis=0,
        tiled=True,
    ).reshape(group_rows, cols)
    group_normed = lax.all_gather(normed, "tp", axis=0, tiled=True)
    table = jnp.dot(spread, columns, preferred_element_type=jnp.float32).astype(jnp.bfloat16)
    slots = table.shape[0]
    arrived = lax.all_to_all(
        table.reshape(groups, -1, cols), "sp", split_axis=0, concat_axis=0, tiled=True
    ).reshape(slots, cols)
    partial = gate_call(arrived, weights)
    partial, group_normed = lax.optimization_barrier((partial, group_normed))
    gated = lax.psum_scatter(partial, "tp", scatter_dimension=0, tiled=False)
    gated = gated.astype(jnp.float32)
    width = gated.shape[1] // 2
    routed_hidden = (jax.nn.silu(gated[:, :width]) * gated[:, width:]).astype(jnp.bfloat16)
    shared_hidden = (
        jax.nn.silu(jnp.dot(group_normed, shared_gate, preferred_element_type=jnp.float32))
        * jnp.dot(group_normed, shared_up, preferred_element_type=jnp.float32)
    ).astype(jnp.bfloat16)
    shared_part = jnp.dot(shared_hidden, shared_down, preferred_element_type=jnp.float32)
    shared_part = shared_part.astype(jnp.bfloat16).reshape(tp_count, rows_here, MODEL_DIM)
    middle = slots // 2
    hidden = [
        lax.all_gather(piece, "tp", axis=0, tiled=False)
        for piece in (routed_hidden[:middle], routed_hidden[middle:])
    ]
    routed_out = down_call(*hidden, weights, cols)
    routed_out, shared_part = lax.optimization_barrier((routed_out, shared_part))
    shared_out = lax.psum_scatter(shared_part, "tp", scatter_dimension=0, tiled=False)
    expert_rows = lax.all_to_all(
        routed_out.reshape(groups, -1, cols), "sp", split_axis=0, concat_axis=0, tiled=True
    ).reshape(slots, cols)
    moe = jnp.dot(share_high, expert_rows, preferred_element_type=jnp.float32) + jnp.dot(
        share_low, expert_rows, preferred_element_type=jnp.float32
    )
    moe = lax.all_to_all(
        moe.astype(jnp.bfloat16).reshape(tp_count, rows_here, cols),
        "tp",
        split_axis=0,
        concat_axis=0,
        tiled=True,
    )
    moe = jnp.concatenate([moe[q] for q in range(tp_count)], axis=1).astype(jnp.float32)
    moe = moe + shared_out.astype(jnp.float32)
    return (mixed.astype(jnp.float32) + rms_scale(moe, moe_gain)).astype(jnp.bfloat16)


def solution(mesh):
    in_specs = (
        P("sp", "tp"),
        P("sp", "tp"),
        P("sp", None),
        P("sp", None),
        P(),
        P(None, "tp"),
        P(None, "tp"),
        P("tp", None),
        P(("sp", "tp"), None),
        P(),
        P(),
        P(("sp", "tp"), None),
        P(("sp", "tp"), None),
        P("sp", None, "tp"),
        P("sp", None, "tp"),
        P("sp", "tp", None),
        P(None, "tp"),
        P(None, "tp"),
        P("tp", None),
        P(),
    )
    out_specs = P(("sp", "tp"), None)
    return jax.shard_map(layer, mesh=mesh, in_specs=in_specs, out_specs=out_specs, check_vma=False)
```

```python
import functools

import jax
import jax.numpy as jnp
from jax import lax
from jax.experimental import pallas as pl
from jax.experimental.pallas import tpu as pltpu
from jax.sharding import PartitionSpec as P


MODEL_DIM = 4096
NOPE_DIM = 64
ROPE_DIM = 32
TOP_K = 2


epsilon = 1e-06
theta_base = 10000.0


def cut_along(array, dim, count):
    before, after = (array.shape[:dim], array.shape[dim + 1 :])
    return jnp.moveaxis(array.reshape(*before, count, -1, *after), dim, 0)


def sum_at_owner(array, axis, dim):
    count = lax.axis_size(axis)
    blocks = lax.all_to_all(cut_along(array, dim, count), axis, 0, 0, tiled=True)
    return jnp.sum(blocks.astype(jnp.float32), axis=0)


def rms_scale(values, gain_vector):
    return (
        values
        * lax.rsqrt(jnp.mean(values * values, axis=-1, keepdims=True) + epsilon)
        * gain_vector
    )


def rotate(values, positions):
    half_dim = values.shape[-1] // 2
    inverse = theta_base ** (-jnp.arange(half_dim, dtype=jnp.float32) / half_dim)
    angles = positions.astype(jnp.float32)[..., None] * inverse
    cosine = jnp.cos(angles)
    sine_part = jnp.sin(angles)
    first_half = values[..., :half_dim]
    second_half = values[..., half_dim:]
    return jnp.concatenate(
        [
            first_half * cosine - second_half * sine_part,
            second_half * cosine + first_half * sine_part,
        ],
        axis=-1,
    )


def project_kernel(own_ref, first_ref, rest_ref, returned_ref, w_ref, out_ref, x_ref):
    pairs = x_ref.shape[1] // 128
    kept = pairs - returned_ref.shape[0]

    @pl.when(pl.program_id(0) == 0)
    def _():
        for pair in range(pairs):
            x = jnp.where(pair < own_ref[0], first_ref[pair], rest_ref[pair])
            if pair >= kept:
                x = jnp.where(pair < own_ref[1], x, returned_ref[pair - kept])
            x_ref[:, pair * 128 : (pair + 1) * 128] = x.astype(jnp.float32).T.astype(jnp.bfloat16)

    out_ref[...] = jnp.dot(x_ref[...], w_ref[...], preferred_element_type=jnp.float32).astype(
        out_ref.dtype
    )


def project_call(own, first, rest, returned, weights):
    depth, cols = weights.shape
    rows = first.shape[2]
    tile = cols // 8
    return pl.pallas_call(
        project_kernel,
        grid=(cols // tile,),
        out_shape=jax.ShapeDtypeStruct((rows, cols), jnp.bfloat16),
        in_specs=[
            pl.BlockSpec(memory_space=pltpu.SMEM),
            pl.BlockSpec(first.shape, lambda n: (0, 0, 0)),
            pl.BlockSpec(rest.shape, lambda n: (0, 0, 0)),
            pl.BlockSpec(returned.shape, lambda n: (0, 0, 0)),
            pl.BlockSpec((depth, tile), lambda n: (0, n)),
        ],
        out_specs=pl.BlockSpec((rows, tile), lambda n: (0, n)),
        scratch_shapes=[pltpu.VMEM((rows, depth), jnp.bfloat16)],
        compiler_params=pltpu.CompilerParams(vmem_limit_bytes=20 * 1024 * 1024),
        cost_estimate=pl.CostEstimate(
            flops=2 * rows * depth * cols, bytes_accessed=11_000_000, transcendentals=0
        ),
    )(own, first, rest, returned, weights)


def pack_kernel(gate_ref, up_ref, down_ref, out_ref):
    cols, width = gate_ref.shape[1], gate_ref.shape[2]
    depth, tile = down_ref.shape[1], out_ref.shape[2]
    out_ref[0, 0:cols, 0:width] = gate_ref[0]
    out_ref[0, 0:cols, width : 2 * width] = up_ref[0]
    for half in range(cols // tile):
        row = cols + half * depth
        out_ref[0, row : row + depth] = down_ref[0, :, half * tile : (half + 1) * tile]


def pack_call(gate, up, down, quarters):
    cols = gate.shape[1] // quarters
    width, depth = gate.shape[2], down.shape[1]
    rows = cols + depth * cols // (2 * width)
    return pl.pallas_call(
        pack_kernel,
        grid=(quarters,),
        out_shape=jax.ShapeDtypeStruct((quarters, rows, 2 * width), gate.dtype),
        in_specs=[
            pl.BlockSpec((1, cols, width), lambda q: (0, q, 0)),
            pl.BlockSpec((1, cols, width), lambda q: (0, q, 0)),
            pl.BlockSpec((1, depth, cols), lambda q: (0, 0, q)),
        ],
        out_specs=pl.BlockSpec((1, rows, 2 * width), lambda q: (q, 0, 0)),
        compiler_params=pltpu.CompilerParams(vmem_limit_bytes=56 * 1024 * 1024),
        cost_estimate=pl.CostEstimate(flops=0, bytes_accessed=13_000_000, transcendentals=0),
    )(gate, up, down)


def gate_kernel(x_ref, w_ref, out_ref):
    out_ref[0] = jnp.dot(x_ref[...], w_ref[0], preferred_element_type=jnp.float32).astype(
        out_ref.dtype
    )


def gate_call(x, weights):
    quarters, _, width = weights.shape
    rows, depth = x.shape
    return pl.pallas_call(
        gate_kernel,
        grid=(quarters,),
        out_shape=jax.ShapeDtypeStruct((quarters, rows, width), jnp.bfloat16),
        in_specs=[
            pl.BlockSpec((rows, depth), lambda q: (0, 0)),
            pl.BlockSpec((1, depth, width), lambda q: (q, 0, 0)),
        ],
        out_specs=pl.BlockSpec((1, rows, width), lambda q: (q, 0, 0)),
        compiler_params=pltpu.CompilerParams(vmem_limit_bytes=56 * 1024 * 1024),
        cost_estimate=pl.CostEstimate(
            flops=2 * rows * depth * width * quarters, bytes_accessed=9_000_000, transcendentals=0
        ),
    )(x, weights)


def down_kernel(first_ref, second_ref, w_ref, routed_ref):
    quarters, middle, _ = first_ref.shape

    def total(ref):
        return sum(
            jnp.dot(ref[q], w_ref[q], preferred_element_type=jnp.float32) for q in range(quarters)
        )

    routed_ref[:middle] = total(first_ref).astype(routed_ref.dtype)
    routed_ref[middle:] = total(second_ref).astype(routed_ref.dtype)


def down_call(first_half, second_half, weights, cols):
    quarters, middle, half = first_half.shape
    tile = weights.shape[2]
    first = weights.shape[1] // half - cols // tile
    return pl.pallas_call(
        down_kernel,
        grid=(cols // tile,),
        out_shape=jax.ShapeDtypeStruct((2 * middle, cols), jnp.bfloat16),
        in_specs=[
            pl.BlockSpec((quarters, middle, half), lambda n: (0, 0, 0)),
            pl.BlockSpec((quarters, middle, half), lambda n: (0, 0, 0)),
            pl.BlockSpec((quarters, half, tile), lambda n: (0, first + n, 0)),
        ],
        out_specs=pl.BlockSpec((2 * middle, tile), lambda n: (0, n)),
        compiler_params=pltpu.CompilerParams(vmem_limit_bytes=24 * 1024 * 1024),
        cost_estimate=pl.CostEstimate(
            flops=4 * middle * half * quarters * cols, bytes_accessed=8_000_000, transcendentals=0
        ),
    )(first_half, second_half, weights)


def slot_tables(routes, weights, experts, capacity):
    blocks, rows, picks = routes.shape
    flat = routes.reshape(blocks, rows * picks)
    onehot = (flat[..., None] == jnp.arange(experts, dtype=jnp.int32)).astype(jnp.int32)
    earlier = jnp.cumsum(onehot, axis=1) - onehot
    target = flat * (blocks * capacity) + jnp.sum(earlier * onehot, axis=-1)
    target = target + jnp.arange(blocks, dtype=jnp.int32)[:, None] * capacity
    target = target.reshape(blocks * rows, picks)
    slots = jnp.arange(experts * blocks * capacity, dtype=jnp.int32)
    spread = jnp.any(target.T[:, None, :] == slots[None, :, None], axis=0).astype(jnp.bfloat16)
    shares = jnp.sum(
        jnp.where(
            target[:, :, None] == slots[None, None, :],
            weights.reshape(blocks * rows, picks)[..., None],
            0.0,
        ),
        axis=1,
    )
    high = lax.reduce_precision(shares, 8, 7)
    return spread, high.astype(jnp.bfloat16), (shares - high).astype(jnp.bfloat16)


def far_pairs(groups, pairs):
    counts = []
    for low in range(groups // 2):
        mine, theirs = low + 5.6, groups + 4.6 - low
        best = min(
            range(pairs // 2 + 1),
            key=lambda n: max(pairs * mine + n * theirs, (pairs - n) * theirs),
        )
        counts.append(best)
    return counts


LOG2E = 1.4426950408889634
PACK_ROWS = 16
CHAINS = (10, 5, 2, 1)
ATTEND_VMEM = 30


def attention_kernel(
    desc_ref, gath_ref, qt_ref, ku_ref, vu_ref, out_ref, rot_ref, w_ref, *, block, score_scale
):
    devices, grows, lat_dim = gath_ref.shape
    rows = grows - PACK_ROWS
    per = block // rows
    width = qt_ref.shape[2]
    half = width // 2
    factor = score_scale * LOG2E
    rot_ref[...] = jnp.zeros_like(rot_ref)

    def unpack(d, _):
        packed = gath_ref[d, rows:grows, :]
        for g in range(rows // PACK_ROWS):
            rot_ref[d, g * PACK_ROWS : (g + 1) * PACK_ROWS, 0:ROPE_DIM] = packed[
                :, g * ROPE_DIM : (g + 1) * ROPE_DIM
            ]
        return 0

    lax.fori_loop(0, devices, unpack, 0)
    n_own, i_own, n_far, i_far = desc_ref[0], desc_ref[1], desc_ref[2], desc_ref[3]
    begin = desc_ref[4]
    pairs = ku_ref.shape[1] // 128
    extra = qt_ref.shape[0] - pairs

    def one_pair(u, _):
        far = u >= n_own
        pair = jnp.where(far, pairs - n_far + (u - n_own), begin + u)
        slot = jnp.where(far, pair + extra, pair)
        index = jnp.where(far, i_far, i_own)
        col = pl.multiple_of(pair * 128, 128)
        w_ref[:, 0:128] = ku_ref[:, pl.ds(col, 128)]
        w_ref[:, 128:256] = vu_ref[:, pl.ds(col, 128)]

        count_all = index + 1
        row = lax.broadcasted_iota(jnp.int32, (block, width), 0)
        lane = lax.broadcasted_iota(jnp.int32, (block, width), 1)
        ahead = row - jnp.where(lane >= half, lane - half, lane) - index * rows
        state = (
            jnp.full((1, width), -1e30, jnp.float32),
            jnp.zeros((1, width), jnp.float32),
            jnp.zeros((128, width), jnp.float32),
        )

        def scores(b):
            lat = gath_ref[pl.ds(b * per, per), 0:rows, :].reshape(block, lat_dim)
            kv = jnp.dot(lat, w_ref[...], preferred_element_type=jnp.float32).astype(jnp.bfloat16)
            rot = rot_ref[pl.ds(b * per, per)].reshape(block, 128)
            keys = jnp.concatenate([kv[:, :128], rot], axis=1)
            s = jnp.dot(keys, qt_ref[slot], preferred_element_type=jnp.float32)
            return jnp.where(ahead <= -b * block, s, -1e30), kv[:, 128:]

        def weigh(v, p):
            return lax.dot_general(
                v,
                p.astype(jnp.bfloat16),
                (((0,), (0,)), ((), ())),
                preferred_element_type=jnp.float32,
            )

        def update(state, s, v):
            top, total, acc = state
            newest = jnp.maximum(top, jnp.max(s, axis=0, keepdims=True))
            alpha = jnp.exp2((top - newest) * factor)
            p = jnp.exp2(s * factor - newest * factor)
            total = total * alpha + jnp.sum(p, axis=0, keepdims=True)
            return newest, total, acc * alpha + weigh(v, p)

        def several(count):
            def body(_, carry):
                start, state = carry
                found = [scores(start + k) for k in range(count)]
                for pair_scores in found:
                    state = update(state, *pair_scores)
                return start + count, state

            return body

        carry, left = (jnp.int32(0), state), count_all
        for count in CHAINS:
            carry = lax.fori_loop(0, left // count, several(count), carry)
            left = left % count
        _, total, acc = carry[1]
        res = acc / total
        out_ref[slot, 0:64, :] = res[0:64, 0:half].astype(jnp.bfloat16)
        out_ref[slot, 64:128, :] = res[64:128, half:].astype(jnp.bfloat16)
        return 0

    lax.fori_loop(0, n_own + n_far, one_pair, 0)


def attention_call(desc, gathered, qt, key_up, value_up, score_scale):
    devices, grows, lat_dim = gathered.shape
    rows = grows - PACK_ROWS
    slots, _, width = qt.shape
    return pl.pallas_call(
        functools.partial(attention_kernel, block=rows, score_scale=score_scale),
        out_shape=jax.ShapeDtypeStruct((slots, 128, width // 2), jnp.bfloat16),
        in_specs=[pl.BlockSpec(memory_space=pltpu.SMEM)]
        + [pl.BlockSpec(memory_space=pltpu.VMEM)] * 4,
        out_specs=pl.BlockSpec(memory_space=pltpu.VMEM),
        scratch_shapes=[
            pltpu.VMEM((devices, rows, 128), jnp.bfloat16),
            pltpu.VMEM((lat_dim, 256), jnp.bfloat16),
        ],
        compiler_params=pltpu.CompilerParams(vmem_limit_bytes=ATTEND_VMEM * 1024 * 1024),
        cost_estimate=pl.CostEstimate(
            flops=50_000_000_000, bytes_accessed=12_000_000, transcendentals=20_000_000
        ),
    )(desc, gathered, qt, key_up, value_up)


def query_tiles(query_nope, query_rot):
    rows = query_nope.shape[0]
    pairs = query_nope.shape[1] // (2 * NOPE_DIM)
    nope = query_nope.reshape(rows, pairs, 2, NOPE_DIM).transpose(1, 2, 3, 0)
    rot = query_rot.reshape(rows, pairs, 2, ROPE_DIM).transpose(1, 2, 3, 0)
    none = jnp.zeros_like(nope[:, 0])
    return jnp.concatenate(
        [
            jnp.concatenate([nope[:, 0], none], axis=2),
            jnp.concatenate([none, nope[:, 1]], axis=2),
            jnp.concatenate([rot[:, 0], rot[:, 1]], axis=2),
            jnp.zeros((pairs, 128 - ROPE_DIM, 2 * rows), query_nope.dtype),
        ],
        axis=1,
    )


def layer(
    query_nope,
    query_rope,
    latent,
    key_rope,
    latent_gain,
    key_up,
    value_up,
    out_proj,
    resid,
    attn_gain,
    pre_gain,
    routes,
    route_weights,
    expert_gate,
    expert_up,
    expert_down,
    shared_gate,
    shared_up,
    shared_down,
    moe_gain,
):
    local_rows = query_nope.shape[0]
    heads_here = query_nope.shape[1] // NOPE_DIM
    query_pos = lax.axis_index("sp") * local_rows + jnp.arange(local_rows, dtype=jnp.int32)
    query_rot = rotate(
        query_rope.astype(jnp.float32).reshape(local_rows, heads_here, ROPE_DIM), query_pos[:, None]
    ).astype(jnp.bfloat16)
    key_rot = rotate(key_rope.astype(jnp.float32), query_pos).astype(jnp.bfloat16)
    latent_normed = rms_scale(latent.astype(jnp.float32), latent_gain).astype(jnp.bfloat16)
    score_scale = (NOPE_DIM + ROPE_DIM) ** (-0.5)

    groups = lax.axis_size("sp")
    place = lax.axis_index("sp").astype(jnp.int32)
    tp_count = lax.axis_size("tp")
    pairs = heads_here // 2
    counts = far_pairs(groups, pairs)
    far = max(1, max(counts))
    cols = MODEL_DIM // tp_count
    rows_here = resid.shape[0]
    capacity = max(2, 2 * rows_here * TOP_K // groups)
    group_rows = tp_count * rows_here

    sent_queries = jnp.concatenate(
        [
            query_nope[:, (pairs - far) * 2 * NOPE_DIM :],
            query_rot.reshape(local_rows, -1)[:, (pairs - far) * 2 * ROPE_DIM :],
        ],
        axis=1,
    )
    down_pairs = [(groups - 1 - low, low) for low in range(groups // 2)]
    far_queries = lax.ppermute(sent_queries, "sp", down_pairs)

    packed_rot = key_rot.reshape(local_rows // PACK_ROWS, PACK_ROWS, ROPE_DIM).transpose(1, 0, 2)
    packed_rot = packed_rot.reshape(PACK_ROWS, -1)
    packed_rot = jnp.pad(packed_rot, ((0, 0), (0, latent.shape[1] - packed_rot.shape[1])))
    gathered = lax.all_gather(
        jnp.concatenate([latent_normed, packed_rot], axis=0), "sp", axis=0, tiled=False
    )

    own_routes = jnp.concatenate([routes.astype(jnp.float32), route_weights], axis=1)
    turn = lax.axis_index("tp")
    parts = [own_routes] + [
        lax.ppermute(own_routes, "tp", [(d, (d + k) % tp_count) for d in range(tp_count)])
        for k in range(1, tp_count)
    ]
    owner = jnp.arange(tp_count, dtype=jnp.int32)[:, None, None]
    route_data = sum(
        jnp.where(owner == (turn - k) % tp_count, part[None], 0.0) for k, part in enumerate(parts)
    )
    packed = pack_call(expert_gate, expert_up, expert_down, tp_count)
    weights = lax.all_to_all(packed, "tp", split_axis=0, concat_axis=0, tiled=True)
    spread, share_high, share_low = slot_tables(
        route_data[..., :TOP_K].astype(jnp.int32), route_data[..., TOP_K:], groups, capacity
    )

    is_low = place < groups // 2
    low_place = jnp.minimum(place, groups - 1 - place)
    moved = jnp.asarray(counts, jnp.int32)[low_place]
    n_own = jnp.where(is_low, pairs, pairs - moved)
    mirror = groups - 1 - place
    early = jnp.where(is_low, 0, moved)
    zero = jnp.zeros_like(place)
    desc = jnp.stack([early, place, jnp.where(is_low, moved, 0), mirror, zero])
    desc_rest = jnp.stack([n_own - early, place, zero, mirror, early])
    tiles = jnp.concatenate(
        [
            query_tiles(query_nope, query_rot),
            query_tiles(
                far_queries[:, : far * 2 * NOPE_DIM], far_queries[:, far * 2 * NOPE_DIM :]
            ),
        ],
        axis=0,
    )
    desc, spread, share_high, share_low = lax.optimization_barrier(
        (desc, spread, share_high, share_low)
    )
    first = attention_call(desc, gathered, tiles, key_up, value_up, score_scale)
    returned = lax.ppermute(first[pairs:], "sp", [(low, high) for high, low in down_pairs])
    desc_rest, first = lax.optimization_barrier((desc_rest, first))
    rest = attention_call(desc_rest, gathered, tiles, key_up, value_up, score_scale)
    partial = project_call(jnp.stack([early, n_own]), first, rest, returned, out_proj)
    projected = sum_at_owner(partial, "tp", 0)
    mixed = (resid.astype(jnp.float32) + rms_scale(projected, attn_gain)).astype(jnp.bfloat16)
    normed = rms_scale(mixed.astype(jnp.float32), pre_gain).astype(jnp.bfloat16)

    columns = lax.all_to_all(
        jnp.stack([normed[:, q * cols : (q + 1) * cols] for q in range(tp_count)]),
        "tp",
        split_axis=0,
        concat_axis=0,
        tiled=True,
    ).reshape(group_rows, cols)
    group_normed = lax.all_gather(normed, "tp", axis=0, tiled=True)
    table = jnp.dot(spread, columns, preferred_element_type=jnp.float32).astype(jnp.bfloat16)
    slots = table.shape[0]
    arrived = lax.all_to_all(
        table.reshape(groups, -1, cols), "sp", split_axis=0, concat_axis=0, tiled=True
    ).reshape(slots, cols)
    partial = gate_call(arrived, weights)
    partial, group_normed = lax.optimization_barrier((partial, group_normed))
    gated = lax.psum_scatter(partial, "tp", scatter_dimension=0, tiled=False)
    gated = gated.astype(jnp.float32)
    width = gated.shape[1] // 2
    routed_hidden = (jax.nn.silu(gated[:, :width]) * gated[:, width:]).astype(jnp.bfloat16)
    shared_hidden = (
        jax.nn.silu(jnp.dot(group_normed, shared_gate, preferred_element_type=jnp.float32))
        * jnp.dot(group_normed, shared_up, preferred_element_type=jnp.float32)
    ).astype(jnp.bfloat16)
    shared_part = jnp.dot(shared_hidden, shared_down, preferred_element_type=jnp.float32)
    shared_part = shared_part.astype(jnp.bfloat16).reshape(tp_count, rows_here, MODEL_DIM)
    middle = slots // 2
    hidden = [
        lax.all_gather(piece, "tp", axis=0, tiled=False)
        for piece in (routed_hidden[:middle], routed_hidden[middle:])
    ]
    hidden, shared_part = lax.optimization_barrier((hidden, shared_part))
    routed_out = down_call(*hidden, weights, cols)
    shared_out = lax.psum_scatter(shared_part, "tp", scatter_dimension=0, tiled=False)
    expert_rows = lax.all_to_all(
        routed_out.reshape(groups, -1, cols), "sp", split_axis=0, concat_axis=0, tiled=True
    ).reshape(slots, cols)
    moe = jnp.dot(share_high, expert_rows, preferred_element_type=jnp.float32) + jnp.dot(
        share_low, expert_rows, preferred_element_type=jnp.float32
    )
    moe = lax.all_to_all(
        moe.astype(jnp.bfloat16).reshape(tp_count, rows_here, cols),
        "tp",
        split_axis=0,
        concat_axis=0,
        tiled=True,
    )
    moe = jnp.concatenate([moe[q] for q in range(tp_count)], axis=1).astype(jnp.float32)
    moe = moe + shared_out.astype(jnp.float32)
    return (mixed.astype(jnp.float32) + rms_scale(moe, moe_gain)).astype(jnp.bfloat16)


def solution(mesh):
    in_specs = (
        P("sp", "tp"),
        P("sp", "tp"),
        P("sp", None),
        P("sp", None),
        P(),
        P(None, "tp"),
        P(None, "tp"),
        P("tp", None),
        P(("sp", "tp"), None),
        P(),
        P(),
        P(("sp", "tp"), None),
        P(("sp", "tp"), None),
        P("sp", None, "tp"),
        P("sp", None, "tp"),
        P("sp", "tp", None),
        P(None, "tp"),
        P(None, "tp"),
        P("tp", None),
        P(),
    )
    out_specs = P(("sp", "tp"), None)
    return jax.shard_map(layer, mesh=mesh, in_specs=in_specs, out_specs=out_specs, check_vma=False)
```
